1024 devices in a mesh: ep: 64 (over z, core), tp: 16 (over y, x).
Axes of the slice: x: 4, y: 4, z: 32, core: 2. Of those that a mesh axis runs over, the one named last changes fastest.
Arguments:
- tokens: bfloat16 [8192, 2048], P('ep'), may hold values from -6 to 6
- chosen: int32 [64, 64, 8], replicated, may hold values from 0 to 127, as said below
- chosen_weight: float32 [64, 64, 8], P('ep'), may hold values from 0.1 to 1
- gate_weight: bfloat16 [64, 2048, 4096], P('ep', None, 'tp'), may hold values from -0.125 to 0.125
- up_weight: bfloat16 [64, 2048, 4096], P('ep', None, 'tp'), may hold values from -0.125 to 0.125
- down_weight: bfloat16 [64, 4096, 2048], P('ep', 'tp'), may hold values from -0.09375 to 0.09375
Outputs:
- combined: bfloat16 [8192, 2048], P('ep', 'tp')
The draws below stay inside these ranges and needn't reach their ends.
Inputs may be any that keep to these rules, and one draw needn't show every extreme that they name: `chosen`: for every block and expert the 8 positions are distinct.
All inputs are finite; a program needn't handle non-finite values.
Results may differ from the reference program's by a relative error of at most 0.015.
Values may be sent and summed in bfloat16 or wider, within the bound.
No kernel may reach another device: no remote copies, remote signals or barrier semaphores. Data moves between devices by JAX's collectives and lax.ppermute only.
A program may use at most 32 MiB of HBM per device.

```python
import jax
import jax.numpy as jnp
from jax import lax

D = 2048
FF = 4096
TOK_DEV = 128
PICK = 8
BLOCKS = 64
EXPERTS = 64
TOKENS = 8192
N_TP = 16


def draw_chosen(key, part):
    keys = jax.random.split(jax.random.fold_in(key, 11), BLOCKS * EXPERTS)
    orders = jax.vmap(lambda single: jax.random.permutation(single, TOK_DEV)[:PICK])(keys)
    return orders.reshape(BLOCKS, EXPERTS, PICK).astype(jnp.int32)


def shard_levels(stream_key, dims, cuts, low, top_value):
    def one(dim, blocks):
        draws = jax.random.uniform(jax.random.fold_in(jax.random.fold_in(stream_key, 6), dim), (blocks,), jnp.float32, low / len(cuts), top_value / len(cuts))
        return jnp.repeat(jnp.exp(draws), dims[dim] // blocks).reshape((-1,) + (1,) * (len(dims) - dim - 1))

    gain = one(*cuts[0])
    for cut in cuts[1:]:
        gain = gain * one(*cut)
    return gain


def gaussian(own_key, extent, width, most, cuts=(), kind=jnp.bfloat16):
    loudness = shard_levels(own_key, extent, cuts, -0.22, 0.18) if cuts else 1.0
    values = jax.random.normal(own_key, extent, jnp.float32) * width * loudness
    return jnp.minimum(jnp.maximum(values, -most), most).astype(kind)


def setup_inputs(seed: int = 0) -> dict:
    splits = jax.random.split(jax.random.key(seed), 7)
    tokens = gaussian(splits[0], (TOKENS, D), 1.0, 6.0, ((0, 64),))
    chosen = draw_chosen(jax.random.fold_in(splits[6], 71), 0)
    chosen_weight = jnp.clip(0.1 + 0.9 * jax.random.uniform(splits[2], (BLOCKS, EXPERTS, PICK), jnp.float32) ** shard_levels(splits[2], (BLOCKS, EXPERTS, PICK), ((0, 64),), -0.2, 0.2), 0.1, 1.0)
    gate_weight = gaussian(splits[3], (EXPERTS, D, FF), D ** -0.5, 0.125, ((0, 64), (2, 16)))
    up_weight = gaussian(splits[4], (EXPERTS, D, FF), D ** -0.5, 0.125, ((0, 64), (2, 16)))
    down_weight = gaussian(splits[5], (EXPERTS, FF, D), FF ** -0.5, 0.09375, ((0, 64), (1, 16)))
    return {"tokens": tokens, "chosen": chosen, "chosen_weight": chosen_weight, "gate_weight": gate_weight, "up_weight": up_weight, "down_weight": down_weight}


def reference(tokens, chosen, chosen_weight, gate_weight, up_weight, down_weight):
    offsets = (jnp.arange(BLOCKS, dtype=jnp.int32) * TOK_DEV)[:, None, None]
    global_rows = (chosen + offsets).astype(jnp.int32)
    per_expert = jnp.transpose(global_rows, (1, 0, 2)).reshape(EXPERTS, BLOCKS * PICK)
    slice_width = FF // N_TP

    def expert_pass(inputs):
        picked, gate_local, up_local, down_local = inputs
        selected = jnp.take(tokens, picked, axis=0)
        gate_sum = jnp.dot(selected, gate_local, preferred_element_type=jnp.float32)
        up_sum = jnp.dot(selected, up_local, preferred_element_type=jnp.float32)
        hidden = (jax.nn.silu(gate_sum) * up_sum).astype(jnp.bfloat16)
        partials = jnp.einsum("rtf,tfd->trd",
                              hidden.reshape(-1, N_TP, slice_width).astype(jnp.float32),
                              down_local.reshape(N_TP, slice_width, D).astype(jnp.float32))
        rounded = lax.optimization_barrier(partials.astype(jnp.bfloat16))
        return jnp.sum(rounded.astype(jnp.float32), axis=0).astype(jnp.bfloat16)

    outputs = lax.map(expert_pass, (per_expert, gate_weight, up_weight, down_weight))
    arranged = jnp.transpose(outputs.reshape(EXPERTS, BLOCKS, PICK, D), (1, 0, 2, 3))
    weighted = arranged.astype(jnp.float32) * chosen_weight[..., None]
    combined = jnp.zeros((BLOCKS * TOK_DEV, D), jnp.float32).at[global_rows.reshape(-1)].add(weighted.reshape(-1, D))
    return combined.astype(jnp.bfloat16)
```

```python
import functools

import jax
import jax.numpy as jnp
from jax import lax
from jax.experimental import pallas as pl
from jax.experimental.pallas import tpu as pltpu
from jax.sharding import PartitionSpec as P

GRID = 4
STEPS = ((0, 1), (0, -1), (1, 0), (-1, 0))
VMEM = pl.BlockSpec(memory_space=pltpu.VMEM)
HBM = pl.BlockSpec(memory_space=pltpu.HBM)


def colour(u):
    return (u // GRID + u % GRID) % 2


def neighbour_pairs(dy, dx):
    return [
        (y * GRID + x, (y + dy) % GRID * GRID + (x + dx) % GRID)
        for y in range(GRID)
        for x in range(GRID)
    ]


def cost(flops, nbytes):
    return pl.CostEstimate(flops=flops, bytes_accessed=nbytes, transcendentals=0)


def in_hbm(array):
    return pltpu.with_memory_space_constraint(array, pltpu.HBM)


def room(mib):
    return pltpu.CompilerParams(vmem_limit_bytes=mib * 2**20)


def pick_kernel(tokens, chosen, out, columns, picks, sems):
    width = out.shape[1]
    start = pl.multiple_of(lax.axis_index("tp") * width, width)
    get_columns = pltpu.make_async_copy(tokens.at[:, pl.ds(start, width)], columns, sems.at[0])
    get_picks = pltpu.make_async_copy(chosen.at[lax.axis_index("ep")], picks, sems.at[1])
    get_columns.start()
    get_picks.start()
    rows = out.shape[0]
    each, experts = picks.shape
    row = lax.broadcasted_iota(jnp.int32, (rows, experts), 0)
    expert = lax.broadcasted_iota(jnp.int32, (rows, experts), 1)
    spread = jnp.where(row // each == expert, 1.0, 0.0).astype(jnp.bfloat16)
    row = lax.broadcasted_iota(jnp.int32, (rows, each), 0)
    pick = lax.broadcasted_iota(jnp.int32, (rows, each), 1)
    mine = row % each == pick
    ones = jnp.ones((each, columns.shape[0]), jnp.bfloat16)
    place = lax.broadcasted_iota(jnp.int32, (rows, columns.shape[0]), 1)
    get_picks.wait()
    all_picks = lax.dot_general(
        spread,
        picks[...].astype(jnp.float32).astype(jnp.bfloat16),
        (((1,), (1,)), ((), ())),
        preferred_element_type=jnp.float32,
    )
    own = jnp.where(mine, all_picks, 0.0).astype(jnp.bfloat16)
    position = jnp.dot(own, ones, preferred_element_type=jnp.float32)
    one_hot = jnp.where(position.astype(jnp.int32) == place, 1.0, 0.0).astype(jnp.bfloat16)
    get_columns.wait()
    out[...] = jnp.dot(one_hot, columns[...], preferred_element_type=jnp.float32).astype(out.dtype)


def place_kernel(chosen, weight, out, picks, sem):
    get_picks = pltpu.make_async_copy(chosen.at[lax.axis_index("ep")], picks, sem)
    get_picks.start()
    each, experts = picks.shape
    tok_count, rows = out.shape[1:]
    row = lax.broadcasted_iota(jnp.int32, (experts, rows), 1)
    expert = lax.broadcasted_iota(jnp.int32, (experts, rows), 0)
    spread = jnp.where(row // each == expert, 1.0, 0.0).astype(jnp.bfloat16)
    row = lax.broadcasted_iota(jnp.int32, (each, rows), 1)
    pick = lax.broadcasted_iota(jnp.int32, (each, rows), 0)
    mine = row % each == pick
    place = lax.broadcasted_iota(jnp.int32, (tok_count, rows), 0)

    def in_row(values):
        every = jnp.dot(values.astype(jnp.bfloat16), spread, preferred_element_type=jnp.float32)
        return jnp.sum(jnp.where(mine, every, 0.0), axis=0, keepdims=True)

    rest = weight[...]
    get_picks.wait()
    here = in_row(picks[...].astype(jnp.float32)).astype(jnp.int32) == place
    for k in range(3):
        term = rest.astype(jnp.bfloat16)
        rest = rest - term.astype(jnp.float32)
        out[k] = jnp.where(here, in_row(term), 0.0).astype(out.dtype)


def combine_kernel(places, rows, out):
    total = jnp.dot(places[0], rows[...], preferred_element_type=jnp.float32)
    for k in range(1, places.shape[0]):
        total += jnp.dot(places[k], rows[...], preferred_element_type=jnp.float32)
    out[...] = total.astype(out.dtype)


def pack_kernel(gate, up, down, *outs):
    depth, units = gate.shape
    part = units // len(outs)
    lanes = 2 * part
    for q, out in enumerate(outs):
        g = gate[:, q * part : (q + 1) * part]
        u = up[:, q * part : (q + 1) * part]
        out[:depth, :] = jnp.concatenate([g, u] if q % 2 == 0 else [u, g], axis=1)
        for c in range(down.shape[1] // lanes):
            out[depth + c * part : depth + (c + 1) * part, :] = down[
                q * part : (q + 1) * part, c * lanes : (c + 1) * lanes
            ]


def spread_kernel(rows, out):
    half = out.shape[1]
    for u in range(out.shape[0]):
        out[u] = rows[colour(u) * half : (colour(u) + 1) * half, :]


def silu(v):
    return v / (1.0 + jnp.exp(-v))


def ffn_kernel(tiles, gate, up, down, p0, p1, p2, p3, out, rows):
    chunks, count, lanes = tiles.shape
    depth, units = gate.shape
    part = units // 4
    for t in range(chunks):
        rows[:, t * lanes : (t + 1) * lanes] = tiles[t]
    low = lax.broadcasted_iota(jnp.int32, (count, lanes), 1) < part
    gate_sum = jnp.dot(rows[...], gate[...], preferred_element_type=jnp.float32)
    up_sum = jnp.dot(rows[...], up[...], preferred_element_type=jnp.float32)
    hidden = [(silu(gate_sum) * up_sum).astype(jnp.bfloat16)]
    for a, b in ((p0, p1), (p2, p3)):
        both = jnp.dot(
            rows[...],
            jnp.concatenate([a[:depth, :], b[:depth, :]], axis=1),
            preferred_element_type=jnp.float32,
        )
        left, right = both[:, :lanes], both[:, lanes:]
        left = silu(left) * pltpu.roll(left, part, 1)
        right = silu(right) * pltpu.roll(right, part, 1)
        hidden.append(jnp.where(low, left, right).astype(jnp.bfloat16))
    hidden = jnp.concatenate(hidden, axis=1)
    for c in range(0, chunks, 2):
        theirs = [
            jnp.concatenate(
                [p[depth + k * part : depth + (k + 1) * part, :] for p in (p0, p1, p2, p3)], axis=0
            )
            for k in (c, c + 1)
        ]
        weights = jnp.concatenate(
            [down[:, c * lanes : (c + 2) * lanes], jnp.concatenate(theirs, axis=1)], axis=0
        )
        sums = jnp.dot(hidden, weights, preferred_element_type=jnp.float32).astype(out.dtype)
        out[c] = sums[:, :lanes]
        out[c + 1] = sums[:, lanes:]


def sum_kernel(parts, out):
    half = parts.shape[1]
    for k in range(2):
        total = None
        for u in range(parts.shape[0]):
            if colour(u) == k:
                term = parts[u].astype(jnp.float32)
                total = term if total is None else total + term
        out[k * half : (k + 1) * half, :] = total.astype(out.dtype)


def exchange(tiles, axis):
    return lax.all_to_all(tiles, axis, split_axis=0, concat_axis=0, tiled=True)


def local(tokens, chosen, chosen_weight, gate_weight, up_weight, down_weight):
    tp_count = lax.axis_size("tp")
    tok_count, model_width = tokens.shape
    blocks, experts, picks_each = chosen.shape
    width = model_width // tp_count
    count = blocks * picks_each
    gate, up, down = gate_weight[0], up_weight[0], down_weight[0]
    units = gate.shape[1]
    bf16 = functools.partial(jax.ShapeDtypeStruct, dtype=jnp.bfloat16)

    by_pick = in_hbm(jnp.transpose(chosen, (0, 2, 1)))
    leaving = pl.pallas_call(
        pick_kernel,
        out_shape=bf16((count, width)),
        in_specs=[HBM, HBM],
        out_specs=VMEM,
        scratch_shapes=[
            pltpu.VMEM((tok_count, width), jnp.bfloat16),
            pltpu.VMEM((picks_each, experts), jnp.int32),
            pltpu.SemaphoreType.DMA((2,)),
        ],
        compiler_params=room(4),
        cost_estimate=cost(2 * count * tok_count * width, 4 * count * width),
        name="pick",
    )(in_hbm(tokens), by_pick)
    arrived = exchange(leaving.reshape(experts, picks_each, width), "ep").reshape(count, width)

    pack = pl.pallas_call(
        pack_kernel,
        out_shape=[bf16((model_width + model_width // 2, units // 2))] * 4,
        in_specs=[VMEM] * 3,
        out_specs=[VMEM] * 4,
        compiler_params=room(12),
        cost_estimate=cost(10**8, 12 * model_width * units),
        name="pack",
    )
    packs = pack(gate, up, down)
    shared = [
        lax.ppermute(pack, "tp", neighbour_pairs(*step))
        for pack, step in zip(packs, STEPS, strict=True)
    ]

    place = pl.pallas_call(
        place_kernel,
        out_shape=bf16((3, tok_count, count)),
        in_specs=[HBM, VMEM],
        out_specs=VMEM,
        scratch_shapes=[pltpu.VMEM((picks_each, experts), jnp.int32), pltpu.SemaphoreType.DMA],
        compiler_params=room(4),
        cost_estimate=cost(10**8, 8 * tok_count * count),
        name="place",
    )
    places = place(by_pick, jnp.transpose(chosen_weight[0]))

    tiles = pl.pallas_call(
        spread_kernel,
        out_shape=bf16((tp_count, count // 2, width)),
        in_specs=[VMEM],
        out_specs=VMEM,
        compiler_params=room(6),
        cost_estimate=cost(10**8, tp_count * count * width),
        name="spread",
    )(arrived)
    tiles = exchange(tiles, "tp")
    partial = pl.pallas_call(
        ffn_kernel,
        out_shape=bf16((tp_count, count // 2, width)),
        in_specs=[VMEM] * 8,
        out_specs=VMEM,
        scratch_shapes=[pltpu.VMEM((count // 2, model_width), jnp.bfloat16)],
        cost_estimate=cost(6 * count * model_width * units, 12 * model_width * units),
        compiler_params=room(20),
        name="ffn",
    )(tiles, gate, up, down, *shared)
    partial = exchange(partial, "tp")
    expert_out = pl.pallas_call(
        sum_kernel,
        out_shape=bf16((count, width)),
        in_specs=[VMEM],
        out_specs=VMEM,
        compiler_params=room(6),
        cost_estimate=cost(10**8, tp_count * count * width),
        name="add",
    )(partial)
    returned = exchange(expert_out.reshape(blocks, picks_each, width), "ep").reshape(
        experts * picks_each, width
    )
    return pl.pallas_call(
        combine_kernel,
        out_shape=bf16((tok_count, width)),
        in_specs=[VMEM] * 2,
        out_specs=VMEM,
        compiler_params=room(4),
        cost_estimate=cost(6 * tok_count * count * width, 8 * tok_count * count),
        name="combine",
    )(places, returned)


def solution(mesh):
    return jax.shard_map(
        local,
        mesh=mesh,
        in_specs=(
            P("ep", None),
            P(),
            P("ep", None, None),
            P("ep", None, "tp"),
            P("ep", None, "tp"),
            P("ep", "tp", None),
        ),
        out_specs=P("ep", "tp"),
        check_vma=False,
    )
```

```python
import functools

import jax
import jax.numpy as jnp
from jax import lax
from jax.experimental import pallas as pl
from jax.experimental.pallas import tpu as pltpu
from jax.sharding import PartitionSpec as P

GRID = 4
STEPS = ((0, 1), (0, -1), (1, 0), (-1, 0))
VMEM = pl.BlockSpec(memory_space=pltpu.VMEM)
HBM = pl.BlockSpec(memory_space=pltpu.HBM)


def colour(u):
    return (u // GRID + u % GRID) % 2


def neighbour_pairs(dy, dx):
    return [
        (y * GRID + x, (y + dy) % GRID * GRID + (x + dx) % GRID)
        for y in range(GRID)
        for x in range(GRID)
    ]


def cost(flops, nbytes):
    return pl.CostEstimate(flops=flops, bytes_accessed=nbytes, transcendentals=0)


def in_hbm(array):
    return pltpu.with_memory_space_constraint(array, pltpu.HBM)


def room(mib):
    return pltpu.CompilerParams(vmem_limit_bytes=mib * 2**20)


def pick_kernel(tokens, chosen, out, columns, picks, sems):
    width = out.shape[1]
    start = pl.multiple_of(lax.axis_index("tp") * width, width)
    get_columns = pltpu.make_async_copy(tokens.at[:, pl.ds(start, width)], columns, sems.at[0])
    get_picks = pltpu.make_async_copy(chosen.at[lax.axis_index("ep")], picks, sems.at[1])
    get_columns.start()
    get_picks.start()
    rows = out.shape[0]
    each, experts = picks.shape
    row = lax.broadcasted_iota(jnp.int32, (rows, experts), 0)
    expert = lax.broadcasted_iota(jnp.int32, (rows, experts), 1)
    spread = jnp.where((row // each + experts // 2) % experts == expert, 1.0, 0.0)
    spread = spread.astype(jnp.bfloat16)
    row = lax.broadcasted_iota(jnp.int32, (rows, each), 0)
    pick = lax.broadcasted_iota(jnp.int32, (rows, each), 1)
    mine = row % each == pick
    ones = jnp.ones((each, columns.shape[0]), jnp.bfloat16)
    place = lax.broadcasted_iota(jnp.int32, (rows, columns.shape[0]), 1)
    get_picks.wait()
    all_picks = lax.dot_general(
        spread,
        picks[...].astype(jnp.float32).astype(jnp.bfloat16),
        (((1,), (1,)), ((), ())),
        preferred_element_type=jnp.float32,
    )
    own = jnp.where(mine, all_picks, 0.0).astype(jnp.bfloat16)
    position = jnp.dot(own, ones, preferred_element_type=jnp.float32)
    one_hot = jnp.where(position.astype(jnp.int32) == place, 1.0, 0.0).astype(jnp.bfloat16)
    get_columns.wait()
    out[...] = jnp.dot(one_hot, columns[...], preferred_element_type=jnp.float32).astype(out.dtype)


def place_kernel(chosen, weight, out, picks, sem):
    get_picks = pltpu.make_async_copy(chosen.at[lax.axis_index("ep")], picks, sem)
    get_picks.start()
    each, experts = picks.shape
    tok_count, rows = out.shape[1:]
    row = lax.broadcasted_iota(jnp.int32, (experts, rows), 1)
    expert = lax.broadcasted_iota(jnp.int32, (experts, rows), 0)
    spread = jnp.where(row // each == expert, 1.0, 0.0).astype(jnp.bfloat16)
    row = lax.broadcasted_iota(jnp.int32, (each, rows), 1)
    pick = lax.broadcasted_iota(jnp.int32, (each, rows), 0)
    mine = row % each == pick
    place = lax.broadcasted_iota(jnp.int32, (tok_count, rows), 0)

    def in_row(values):
        every = jnp.dot(values.astype(jnp.bfloat16), spread, preferred_element_type=jnp.float32)
        return jnp.sum(jnp.where(mine, every, 0.0), axis=0, keepdims=True)

    rest = weight[...]
    get_picks.wait()
    here = in_row(picks[...].astype(jnp.float32)).astype(jnp.int32) == place
    for k in range(3):
        term = rest.astype(jnp.bfloat16)
        rest = rest - term.astype(jnp.float32)
        out[k] = jnp.where(here, in_row(term), 0.0).astype(out.dtype)


def combine_kernel(places, rows, out):
    total = jnp.dot(places[0], rows[...], preferred_element_type=jnp.float32)
    for k in range(1, places.shape[0]):
        total += jnp.dot(places[k], rows[...], preferred_element_type=jnp.float32)
    out[...] = total.astype(out.dtype)


def pack_kernel(gate, up, down, *outs):
    depth, units = gate.shape
    part = units // len(outs)
    lanes = 2 * part
    for q, out in enumerate(outs):
        g = gate[:, q * part : (q + 1) * part]
        u = up[:, q * part : (q + 1) * part]
        out[:depth, :] = jnp.concatenate([g, u] if q % 2 == 0 else [u, g], axis=1)
        for c in range(down.shape[1] // lanes):
            out[depth + c * part : depth + (c + 1) * part, :] = down[
                q * part : (q + 1) * part, c * lanes : (c + 1) * lanes
            ]


def spread_kernel(rows, out):
    half = out.shape[1]
    for u in range(out.shape[0]):
        out[u] = rows[colour(u) * half : (colour(u) + 1) * half, :]


def silu(v):
    return v / (1.0 + jnp.exp(-v))


def ffn_kernel(tiles, gate, up, down, p0, p1, p2, p3, out, rows):
    chunks, count, lanes = tiles.shape
    depth, units = gate.shape
    part = units // 4
    for t in range(chunks):
        rows[:, t * lanes : (t + 1) * lanes] = tiles[t]
    low = lax.broadcasted_iota(jnp.int32, (count, lanes), 1) < part
    gate_sum = jnp.dot(rows[...], gate[...], preferred_element_type=jnp.float32)
    up_sum = jnp.dot(rows[...], up[...], preferred_element_type=jnp.float32)
    hidden = [(silu(gate_sum) * up_sum).astype(jnp.bfloat16)]
    for a, b in ((p0, p1), (p2, p3)):
        both = jnp.dot(
            rows[...],
            jnp.concatenate([a[:depth, :], b[:depth, :]], axis=1),
            preferred_element_type=jnp.float32,
        )
        left, right = both[:, :lanes], both[:, lanes:]
        left = silu(left) * pltpu.roll(left, part, 1)
        right = silu(right) * pltpu.roll(right, part, 1)
        hidden.append(jnp.where(low, left, right).astype(jnp.bfloat16))
    hidden = jnp.concatenate(hidden, axis=1)
    for c in range(0, chunks, 2):
        theirs = [
            jnp.concatenate(
                [p[depth + k * part : depth + (k + 1) * part, :] for p in (p0, p1, p2, p3)], axis=0
            )
            for k in (c, c + 1)
        ]
        weights = jnp.concatenate(
            [down[:, c * lanes : (c + 2) * lanes], jnp.concatenate(theirs, axis=1)], axis=0
        )
        sums = jnp.dot(hidden, weights, preferred_element_type=jnp.float32).astype(out.dtype)
        out[c] = sums[:, :lanes]
        out[c + 1] = sums[:, lanes:]


def sum_kernel(parts, out):
    half = parts.shape[1]
    for k in range(2):
        total = None
        for u in range(parts.shape[0]):
            if colour(u) == k:
                term = parts[u].astype(jnp.float32)
                total = term if total is None else total + term
        out[(1 - k) * half : (2 - k) * half, :] = total.astype(out.dtype)


def exchange(tiles, axis, first=0):
    size = lax.axis_size(axis)
    groups = [[(i + first) % size for i in range(size)]] if first else None
    return lax.all_to_all(
        tiles, axis, split_axis=0, concat_axis=0, axis_index_groups=groups, tiled=True
    )


def local(tokens, chosen, chosen_weight, gate_weight, up_weight, down_weight):
    tp_count = lax.axis_size("tp")
    tok_count, model_width = tokens.shape
    blocks, experts, picks_each = chosen.shape
    width = model_width // tp_count
    count = blocks * picks_each
    gate, up, down = gate_weight[0], up_weight[0], down_weight[0]
    units = gate.shape[1]
    bf16 = functools.partial(jax.ShapeDtypeStruct, dtype=jnp.bfloat16)

    by_pick = in_hbm(jnp.transpose(chosen, (0, 2, 1)))
    leaving = pl.pallas_call(
        pick_kernel,
        out_shape=bf16((count, width)),
        in_specs=[HBM, HBM],
        out_specs=VMEM,
        scratch_shapes=[
            pltpu.VMEM((tok_count, width), jnp.bfloat16),
            pltpu.VMEM((picks_each, experts), jnp.int32),
            pltpu.SemaphoreType.DMA((2,)),
        ],
        compiler_params=room(4),
        cost_estimate=cost(2 * count * tok_count * width, 4 * count * width),
        name="pick",
    )(in_hbm(tokens), by_pick)
    arrived = exchange(
        leaving.reshape(experts, picks_each, width), "ep", experts // 2
    ).reshape(count, width)

    pack = pl.pallas_call(
        pack_kernel,
        out_shape=[bf16((model_width + model_width // 2, units // 2))] * 4,
        in_specs=[VMEM] * 3,
        out_specs=[VMEM] * 4,
        compiler_params=room(12),
        cost_estimate=cost(10**8, 12 * model_width * units),
        name="pack",
    )
    packs = pack(gate, up, down)
    shared = [
        lax.ppermute(pack, "tp", neighbour_pairs(*step))
        for pack, step in zip(packs, STEPS, strict=True)
    ]

    place = pl.pallas_call(
        place_kernel,
        out_shape=bf16((3, tok_count, count)),
        in_specs=[HBM, VMEM],
        out_specs=VMEM,
        scratch_shapes=[pltpu.VMEM((picks_each, experts), jnp.int32), pltpu.SemaphoreType.DMA],
        compiler_params=room(4),
        cost_estimate=cost(10**8, 8 * tok_count * count),
        name="place",
    )
    places = place(by_pick, jnp.transpose(chosen_weight[0]))

    tiles = pl.pallas_call(
        spread_kernel,
        out_shape=bf16((tp_count, count // 2, width)),
        in_specs=[VMEM],
        out_specs=VMEM,
        compiler_params=room(6),
        cost_estimate=cost(10**8, tp_count * count * width),
        name="spread",
    )(arrived)
    tiles = exchange(tiles, "tp")
    partial = pl.pallas_call(
        ffn_kernel,
        out_shape=bf16((tp_count, count // 2, width)),
        in_specs=[VMEM] * 8,
        out_specs=VMEM,
        scratch_shapes=[pltpu.VMEM((count // 2, model_width), jnp.bfloat16)],
        cost_estimate=cost(6 * count * model_width * units, 12 * model_width * units),
        compiler_params=room(20),
        name="ffn",
    )(tiles, gate, up, down, *shared)
    partial = exchange(partial, "tp")
    expert_out = pl.pallas_call(
        sum_kernel,
        out_shape=bf16((count, width)),
        in_specs=[VMEM],
        out_specs=VMEM,
        compiler_params=room(6),
        cost_estimate=cost(10**8, tp_count * count * width),
        name="add",
    )(partial)
    returned = exchange(expert_out.reshape(blocks, picks_each, width), "ep").reshape(
        experts * picks_each, width
    )
    return pl.pallas_call(
        combine_kernel,
        out_shape=bf16((tok_count, width)),
        in_specs=[VMEM] * 2,
        out_specs=VMEM,
        compiler_params=room(4),
        cost_estimate=cost(6 * tok_count * count * width, 8 * tok_count * count),
        name="combine",
    )(places, returned)


def solution(mesh):
    return jax.shard_map(
        local,
        mesh=mesh,
        in_specs=(
            P("ep", None),
            P(),
            P("ep", None, None),
            P("ep", None, "tp"),
            P("ep", None, "tp"),
            P("ep", "tp", None),
        ),
        out_specs=P("ep", "tp"),
        check_vma=False,
    )
```

```python
import functools

import jax
import jax.numpy as jnp
from jax import lax
from jax.experimental import pallas as pl
from jax.experimental.pallas import tpu as pltpu
from jax.sharding import PartitionSpec as P

GRID = 4
STEPS = ((0, 1), (0, -1), (1, 0), (-1, 0))
VMEM = pl.BlockSpec(memory_space=pltpu.VMEM)
LEAD_OUT, LEAD_BACK = 1 / 4, 1 / 2
HBM = pl.BlockSpec(memory_space=pltpu.HBM)


def colour(u):
    return (u // GRID + u % GRID) % 2


def neighbour_pairs(dy, dx):
    return [
        (y * GRID + x, (y + dy) % GRID * GRID + (x + dx) % GRID)
        for y in range(GRID)
        for x in range(GRID)
    ]


def cost(flops, nbytes):
    return pl.CostEstimate(flops=flops, bytes_accessed=nbytes, transcendentals=0)


def in_hbm(array):
    return pltpu.with_memory_space_constraint(array, pltpu.HBM)


def room(mib):
    return pltpu.CompilerParams(vmem_limit_bytes=mib * 2**20)


def pick_kernel(first, tokens, chosen, out, columns, picks, sems):
    width = out.shape[1]
    start = pl.multiple_of(lax.axis_index("tp") * width, width)
    get_columns = pltpu.make_async_copy(tokens.at[:, pl.ds(start, width)], columns, sems.at[0])
    get_picks = pltpu.make_async_copy(chosen.at[lax.axis_index("ep")], picks, sems.at[1])
    get_columns.start()
    get_picks.start()
    rows = out.shape[0]
    each, experts = picks.shape
    row = lax.broadcasted_iota(jnp.int32, (rows, experts), 0)
    expert = lax.broadcasted_iota(jnp.int32, (rows, experts), 1)
    spread = jnp.where((row // each + first) % experts == expert, 1.0, 0.0)
    spread = spread.astype(jnp.bfloat16)
    row = lax.broadcasted_iota(jnp.int32, (rows, each), 0)
    pick = lax.broadcasted_iota(jnp.int32, (rows, each), 1)
    mine = row % each == pick
    ones = jnp.ones((each, columns.shape[0]), jnp.bfloat16)
    place = lax.broadcasted_iota(jnp.int32, (rows, columns.shape[0]), 1)
    get_picks.wait()
    all_picks = lax.dot_general(
        spread,
        picks[...].astype(jnp.float32).astype(jnp.bfloat16),
        (((1,), (1,)), ((), ())),
        preferred_element_type=jnp.float32,
    )
    own = jnp.where(mine, all_picks, 0.0).astype(jnp.bfloat16)
    position = jnp.dot(own, ones, preferred_element_type=jnp.float32)
    one_hot = jnp.where(position.astype(jnp.int32) == place, 1.0, 0.0).astype(jnp.bfloat16)
    get_columns.wait()
    out[...] = jnp.dot(one_hot, columns[...], preferred_element_type=jnp.float32).astype(out.dtype)


def place_kernel(first, chosen, weight, out, picks, sem):
    get_picks = pltpu.make_async_copy(chosen.at[lax.axis_index("ep")], picks, sem)
    get_picks.start()
    each, experts = picks.shape
    tok_count, rows = out.shape[1:]
    row = lax.broadcasted_iota(jnp.int32, (experts, rows), 1)
    expert = lax.broadcasted_iota(jnp.int32, (experts, rows), 0)
    spread = jnp.where((row // each + first) % experts == expert, 1.0, 0.0)
    spread = spread.astype(jnp.bfloat16)
    row = lax.broadcasted_iota(jnp.int32, (each, rows), 1)
    pick = lax.broadcasted_iota(jnp.int32, (each, rows), 0)
    mine = row % each == pick
    place = lax.broadcasted_iota(jnp.int32, (tok_count, rows), 0)

    def in_row(values):
        every = jnp.dot(values.astype(jnp.bfloat16), spread, preferred_element_type=jnp.float32)
        return jnp.sum(jnp.where(mine, every, 0.0), axis=0, keepdims=True)

    rest = weight[...]
    get_picks.wait()
    here = in_row(picks[...].astype(jnp.float32)).astype(jnp.int32) == place
    for k in range(3):
        term = rest.astype(jnp.bfloat16)
        rest = rest - term.astype(jnp.float32)
        out[k] = jnp.where(here, in_row(term), 0.0).astype(out.dtype)


def combine_kernel(places, rows, out):
    total = jnp.dot(places[0], rows[...], preferred_element_type=jnp.float32)
    for k in range(1, places.shape[0]):
        total += jnp.dot(places[k], rows[...], preferred_element_type=jnp.float32)
    out[...] = total.astype(out.dtype)


def pack_kernel(gate_hbm, up_hbm, down_hbm, *refs):
    outs, (gate, up, down, packed, loads, stores) = refs[:4], refs[4:]
    into = [
        pltpu.make_async_copy(src, dst, loads.at[k])
        for k, (src, dst) in enumerate(((gate_hbm, gate), (up_hbm, up), (down_hbm, down)))
    ]
    for copy in into:
        copy.start()
    depth, units = gate.shape
    part = units // len(outs)
    lanes = 2 * part
    for copy in into:
        copy.wait()
    leave = []
    for q, out in enumerate(outs):
        g = gate[:, q * part : (q + 1) * part]
        u = up[:, q * part : (q + 1) * part]
        packed[q, :depth, :] = jnp.concatenate([g, u] if q % 2 == 0 else [u, g], axis=1)
        for c in range(down.shape[1] // lanes):
            packed[q, depth + c * part : depth + (c + 1) * part, :] = down[
                q * part : (q + 1) * part, c * lanes : (c + 1) * lanes
            ]
        leave.append(pltpu.make_async_copy(packed.at[q], out, stores.at[q]))
        leave[-1].start()
    for copy in leave:
        copy.wait()


def spread_kernel(rows, out):
    half = out.shape[1]
    for u in range(out.shape[0]):
        out[u] = rows[colour(u) * half : (colour(u) + 1) * half, :]


def silu(v):
    return v / (1.0 + jnp.exp(-v))


def ffn_kernel(tiles, gate, up, down, p0, p1, p2, p3, out, rows):
    chunks, count, lanes = tiles.shape
    depth, units = gate.shape
    part = units // 4
    for t in range(chunks):
        rows[:, t * lanes : (t + 1) * lanes] = tiles[t]
    low = lax.broadcasted_iota(jnp.int32, (count, lanes), 1) < part
    gate_sum = jnp.dot(rows[...], gate[...], preferred_element_type=jnp.float32)
    up_sum = jnp.dot(rows[...], up[...], preferred_element_type=jnp.float32)
    hidden = [(silu(gate_sum) * up_sum).astype(jnp.bfloat16)]
    for a, b in ((p0, p1), (p2, p3)):
        both = jnp.dot(
            rows[...],
            jnp.concatenate([a[:depth, :], b[:depth, :]], axis=1),
            preferred_element_type=jnp.float32,
        )
        left, right = both[:, :lanes], both[:, lanes:]
        left = silu(left) * pltpu.roll(left, part, 1)
        right = silu(right) * pltpu.roll(right, part, 1)
        hidden.append(jnp.where(low, left, right).astype(jnp.bfloat16))
    hidden = jnp.concatenate(hidden, axis=1)
    for c in range(0, chunks, 2):
        theirs = [
            jnp.concatenate(
                [p[depth + k * part : depth + (k + 1) * part, :] for p in (p0, p1, p2, p3)], axis=0
            )
            for k in (c, c + 1)
        ]
        weights = jnp.concatenate(
            [down[:, c * lanes : (c + 2) * lanes], jnp.concatenate(theirs, axis=1)], axis=0
        )
        sums = jnp.dot(hidden, weights, preferred_element_type=jnp.float32).astype(out.dtype)
        out[c] = sums[:, :lanes]
        out[c + 1] = sums[:, lanes:]


def sum_kernel(shift, parts, out):
    half, rows = parts.shape[1], out.shape[0]
    for k in range(2):
        total = None
        for u in range(parts.shape[0]):
            if colour(u) == k:
                term = parts[u].astype(jnp.float32)
                total = term if total is None else total + term
        for r in range(0, half, shift):
            to = (k * half + r - shift) % rows
            out[to : to + shift, :] = total[r : r + shift, :].astype(out.dtype)


def exchange(tiles, axis, first=0):
    size = lax.axis_size(axis)
    groups = [[(i + first) % size for i in range(size)]] if first else None
    return lax.all_to_all(
        tiles, axis, split_axis=0, concat_axis=0, axis_index_groups=groups, tiled=True
    )


def local(tokens, chosen, chosen_weight, gate_weight, up_weight, down_weight):
    tp_count = lax.axis_size("tp")
    tok_count, model_width = tokens.shape
    blocks, experts, picks_each = chosen.shape
    width = model_width // tp_count
    count = blocks * picks_each
    out_first, back_first = int(LEAD_OUT * experts), int(LEAD_BACK * experts)
    gate, up, down = gate_weight[0], up_weight[0], down_weight[0]
    units = gate.shape[1]
    bf16 = functools.partial(jax.ShapeDtypeStruct, dtype=jnp.bfloat16)

    by_pick = in_hbm(jnp.transpose(chosen, (0, 2, 1)))
    leaving = pl.pallas_call(
        functools.partial(pick_kernel, out_first),
        out_shape=bf16((count, width)),
        in_specs=[HBM, HBM],
        out_specs=VMEM,
        scratch_shapes=[
            pltpu.VMEM((tok_count, width), jnp.bfloat16),
            pltpu.VMEM((picks_each, experts), jnp.int32),
            pltpu.SemaphoreType.DMA((2,)),
        ],
        compiler_params=room(4),
        cost_estimate=cost(2 * count * tok_count * width, 4 * count * width),
        name="pick",
    )(in_hbm(tokens), by_pick)
    arrived = exchange(
        leaving.reshape(experts, picks_each, width), "ep", out_first
    ).reshape(count, width)

    pack = pl.pallas_call(
        pack_kernel,
        out_shape=[bf16((model_width + model_width // 2, units // 2))] * 4,
        in_specs=[HBM] * 3,
        out_specs=[HBM] * 4,
        scratch_shapes=[
            pltpu.VMEM(gate.shape, jnp.bfloat16),
            pltpu.VMEM(up.shape, jnp.bfloat16),
            pltpu.VMEM(down.shape, jnp.bfloat16),
            pltpu.VMEM((4, model_width + model_width // 2, units // 2), jnp.bfloat16),
            pltpu.SemaphoreType.DMA((3,)),
            pltpu.SemaphoreType.DMA((4,)),
        ],
        compiler_params=room(12),
        cost_estimate=cost(10**8, 12 * model_width * units),
        name="pack",
    )
    packs = pack(in_hbm(gate), in_hbm(up), in_hbm(down))
    shared = [
        lax.ppermute(pack, "tp", neighbour_pairs(*step))
        for pack, step in zip(packs, STEPS, strict=True)
    ]

    place = pl.pallas_call(
        functools.partial(place_kernel, back_first),
        out_shape=bf16((3, tok_count, count)),
        in_specs=[HBM, VMEM],
        out_specs=VMEM,
        scratch_shapes=[pltpu.VMEM((picks_each, experts), jnp.int32), pltpu.SemaphoreType.DMA],
        compiler_params=room(4),
        cost_estimate=cost(10**8, 8 * tok_count * count),
        name="place",
    )
    places = place(by_pick, jnp.transpose(chosen_weight[0]))

    tiles = pl.pallas_call(
        spread_kernel,
        out_shape=bf16((tp_count, count // 2, width)),
        in_specs=[VMEM],
        out_specs=VMEM,
        compiler_params=room(6),
        cost_estimate=cost(10**8, tp_count * count * width),
        name="spread",
    )(arrived)
    tiles = exchange(tiles, "tp")
    partial = pl.pallas_call(
        ffn_kernel,
        out_shape=bf16((tp_count, count // 2, width)),
        in_specs=[VMEM] * 8,
        out_specs=VMEM,
        scratch_shapes=[pltpu.VMEM((count // 2, model_width), jnp.bfloat16)],
        cost_estimate=cost(6 * count * model_width * units, 12 * model_width * units),
        compiler_params=room(20),
        name="ffn",
    )(tiles, gate, up, down, *shared)
    partial = exchange(partial, "tp")
    expert_out = pl.pallas_call(
        functools.partial(sum_kernel, (back_first - out_first) * picks_each),
        out_shape=bf16((count, width)),
        in_specs=[VMEM],
        out_specs=VMEM,
        compiler_params=room(6),
        cost_estimate=cost(10**8, tp_count * count * width),
        name="add",
    )(partial)
    returned = exchange(
        expert_out.reshape(blocks, picks_each, width), "ep", back_first
    ).reshape(experts * picks_each, width)
    return pl.pallas_call(
        combine_kernel,
        out_shape=bf16((tok_count, width)),
        in_specs=[VMEM] * 2,
        out_specs=VMEM,
        compiler_params=room(4),
        cost_estimate=cost(6 * tok_count * count * width, 8 * tok_count * count),
        name="combine",
    )(places, returned)


def solution(mesh):
    return jax.shard_map(
        local,
        mesh=mesh,
        in_specs=(
            P("ep", None),
            P(),
            P("ep", None, None),
            P("ep", None, "tp"),
            P("ep", None, "tp"),
            P("ep", "tp", None),
        ),
        out_specs=P("ep", "tp"),
        check_vma=False,
    )
```

```python
import functools

import jax
import jax.numpy as jnp
from jax import lax
from jax.experimental import pallas as pl
from jax.experimental.pallas import tpu as pltpu
from jax.sharding import PartitionSpec as P

GRID = 4
STEPS = (((0, 1), (0, -1)), ((1, 0), (-1, 0)))
VMEM = pl.BlockSpec(memory_space=pltpu.VMEM)
LEAD_OUT, LEAD_BACK = 1 / 2, 1 / 2
ANY = pl.BlockSpec(memory_space=pl.ANY)
HBM = pl.BlockSpec(memory_space=pltpu.HBM)


def colour(u):
    return (u // GRID + u % GRID) % 2


def neighbour_pairs(which, ep_count):
    pairs = []
    for e in range(ep_count):
        dy, dx = STEPS[e % 2][which]
        for y in range(GRID):
            for x in range(GRID):
                to = (y + dy) % GRID * GRID + (x + dx) % GRID
                pairs.append((e * GRID**2 + y * GRID + x, e * GRID**2 + to))
    return pairs


def cost(flops, nbytes):
    return pl.CostEstimate(flops=flops, bytes_accessed=nbytes, transcendentals=0)


def in_hbm(array):
    return pltpu.with_memory_space_constraint(array, pltpu.HBM)


def room(mib):
    return pltpu.CompilerParams(vmem_limit_bytes=mib * 2**20)


def pick_kernel(first, tokens, chosen, out, columns, picks, sems):
    width = out.shape[1]
    start = pl.multiple_of(lax.axis_index("tp") * width, width)
    get_columns = pltpu.make_async_copy(tokens.at[:, pl.ds(start, width)], columns, sems.at[0])
    get_picks = pltpu.make_async_copy(chosen.at[lax.axis_index("ep")], picks, sems.at[1])
    get_columns.start()
    get_picks.start()
    rows = out.shape[0]
    each, experts = picks.shape
    row = lax.broadcasted_iota(jnp.int32, (rows, experts), 0)
    expert = lax.broadcasted_iota(jnp.int32, (rows, experts), 1)
    spread = jnp.where((row // each + first) % experts == expert, 1.0, 0.0)
    spread = spread.astype(jnp.bfloat16)
    row = lax.broadcasted_iota(jnp.int32, (rows, each), 0)
    pick = lax.broadcasted_iota(jnp.int32, (rows, each), 1)
    mine = row % each == pick
    ones = jnp.ones((each, columns.shape[0]), jnp.bfloat16)
    place = lax.broadcasted_iota(jnp.int32, (rows, columns.shape[0]), 1)
    get_picks.wait()
    all_picks = lax.dot_general(
        spread,
        picks[...].astype(jnp.float32).astype(jnp.bfloat16),
        (((1,), (1,)), ((), ())),
        preferred_element_type=jnp.float32,
    )
    own = jnp.where(mine, all_picks, 0.0).astype(jnp.bfloat16)
    position = jnp.dot(own, ones, preferred_element_type=jnp.float32)
    one_hot = jnp.where(position.astype(jnp.int32) == place, 1.0, 0.0).astype(jnp.bfloat16)
    get_columns.wait()
    out[...] = jnp.dot(one_hot, columns[...], preferred_element_type=jnp.float32).astype(out.dtype)


def place_kernel(first, chosen, weight, out, picks, sem):
    get_picks = pltpu.make_async_copy(chosen.at[lax.axis_index("ep")], picks, sem)
    get_picks.start()
    each, experts = picks.shape
    tok_count, rows = out.shape[1:]
    row = lax.broadcasted_iota(jnp.int32, (experts, rows), 1)
    expert = lax.broadcasted_iota(jnp.int32, (experts, rows), 0)
    spread = jnp.where((row // each + first) % experts == expert, 1.0, 0.0)
    spread = spread.astype(jnp.bfloat16)
    row = lax.broadcasted_iota(jnp.int32, (each, rows), 1)
    pick = lax.broadcasted_iota(jnp.int32, (each, rows), 0)
    mine = row % each == pick
    place = lax.broadcasted_iota(jnp.int32, (tok_count, rows), 0)

    def in_row(values):
        every = jnp.dot(values.astype(jnp.bfloat16), spread, preferred_element_type=jnp.float32)
        return jnp.sum(jnp.where(mine, every, 0.0), axis=0, keepdims=True)

    rest = weight[...]
    get_picks.wait()
    here = in_row(picks[...].astype(jnp.float32)).astype(jnp.int32) == place
    for k in range(3):
        term = rest.astype(jnp.bfloat16)
        rest = rest - term.astype(jnp.float32)
        out[k] = jnp.where(here, in_row(term), 0.0).astype(out.dtype)


def combine_kernel(places, rows, out):
    total = jnp.dot(places[0], rows[...], preferred_element_type=jnp.float32)
    for k in range(1, places.shape[0]):
        total += jnp.dot(places[k], rows[...], preferred_element_type=jnp.float32)
    out[...] = total.astype(out.dtype)


def pack_kernel(gate, up, down, *refs):
    outs, (packed, loads, stores) = refs[:2], refs[2:]
    depth, units = gate.shape
    part = units // 2
    into = []
    for q in range(2):
        mine = pl.ds(q * part, part)
        target = packed.at[q]
        top = pl.ds(0, depth)
        copies = [
            (gate.at[:, mine], target.at[top, pl.ds(0, part)]),
            (up.at[:, mine], target.at[top, pl.ds(part, part)]),
        ]
        for c in range(depth // units):
            copies.append(
                (
                    down.at[mine, pl.ds(c * units, units)],
                    target.at[pl.ds(depth + c * part, part), :],
                )
            )
        into.append([pltpu.make_async_copy(*ends, loads.at[q, k]) for k, ends in enumerate(copies)])
    for copies in into:
        for copy in copies:
            copy.start()
    leave = []
    for q, out in enumerate(outs):
        for copy in into[q]:
            copy.wait()
        leave.append(pltpu.make_async_copy(packed.at[q], out, stores.at[q]))
        leave[-1].start()
    for copy in leave:
        copy.wait()


def spread_kernel(rows, out, stores):
    half = out.shape[1]
    copies = [
        pltpu.make_async_copy(rows.at[pl.ds(colour(u) * half, half), :], out.at[u], stores.at[u])
        for u in range(out.shape[0])
    ]
    for copy in copies:
        copy.start()
    for copy in copies:
        copy.wait()


def silu(v):
    return v / (1.0 + jnp.exp(-v))


def ffn_kernel(tiles, gate, up, d_hbm, p0_hbm, p1_hbm, out, rows, p0, p1, down, row_sems, p_sems):
    chunks, _, lanes = tiles.shape
    depth, units = gate.shape
    part = units // 2
    get_rows = [
        pltpu.make_async_copy(tiles.at[t], rows.at[:, pl.ds(t * lanes, lanes)], row_sems.at[t])
        for t in range(chunks)
    ]
    get_shared = [
        pltpu.make_async_copy(src, dst, p_sems.at[k])
        for k, (src, dst) in enumerate(((p0_hbm, p0), (p1_hbm, p1), (d_hbm, down)))
    ]
    for copy in get_rows + get_shared:
        copy.start()
    for copy in get_rows:
        copy.wait()
    gate_sum = jnp.dot(rows[...], gate[...], preferred_element_type=jnp.float32)
    up_sum = jnp.dot(rows[...], up[...], preferred_element_type=jnp.float32)
    hidden = [(silu(gate_sum) * up_sum).astype(jnp.bfloat16)]
    for p, copy in zip((p0, p1), get_shared[:2], strict=True):
        copy.wait()
        both = jnp.dot(rows[...], p[:depth, :], preferred_element_type=jnp.float32)
        hidden.append((silu(both[:, :part]) * both[:, part:]).astype(jnp.bfloat16))
    hidden = jnp.concatenate(hidden, axis=1)
    get_shared[2].wait()
    for c in range(depth // units):
        theirs = pl.ds(depth + c * part, part)
        weights = jnp.concatenate(
            [down[:, c * units : (c + 1) * units], p0[theirs, :], p1[theirs, :]], axis=0
        )
        sums = jnp.dot(hidden, weights, preferred_element_type=jnp.float32).astype(out.dtype)
        for k in range(units // lanes):
            out[c * (units // lanes) + k] = sums[:, k * lanes : (k + 1) * lanes]


def sum_kernel(shift, parts, out):
    half, rows = parts.shape[1], out.shape[0]
    for k in range(2):
        total = None
        for u in range(parts.shape[0]):
            if colour(u) == k:
                term = parts[u].astype(jnp.float32)
                total = term if total is None else total + term
        step = shift or half
        for r in range(0, half, step):
            to = (k * half + r - shift) % rows
            out[to : to + step, :] = total[r : r + step, :].astype(out.dtype)


def exchange(tiles, axis, first=0):
    size = lax.axis_size(axis)
    groups = [[(i + first) % size for i in range(size)]] if first else None
    return lax.all_to_all(
        tiles, axis, split_axis=0, concat_axis=0, axis_index_groups=groups, tiled=True
    )


def local(tokens, chosen, chosen_weight, gate_weight, up_weight, down_weight):
    tp_count = lax.axis_size("tp")
    tok_count, model_width = tokens.shape
    blocks, experts, picks_each = chosen.shape
    width = model_width // tp_count
    count = blocks * picks_each
    out_first, back_first = int(LEAD_OUT * experts), int(LEAD_BACK * experts)
    gate, up, down = gate_weight[0], up_weight[0], down_weight[0]
    units = gate.shape[1]
    bf16 = functools.partial(jax.ShapeDtypeStruct, dtype=jnp.bfloat16)

    by_pick = in_hbm(jnp.transpose(chosen, (0, 2, 1)))
    leaving = pl.pallas_call(
        functools.partial(pick_kernel, out_first),
        out_shape=bf16((count, width)),
        in_specs=[HBM, HBM],
        out_specs=VMEM,
        scratch_shapes=[
            pltpu.VMEM((tok_count, width), jnp.bfloat16),
            pltpu.VMEM((picks_each, experts), jnp.int32),
            pltpu.SemaphoreType.DMA((2,)),
        ],
        compiler_params=room(4),
        cost_estimate=cost(2 * count * tok_count * width, 4 * count * width),
        name="pick",
    )(in_hbm(tokens), by_pick)
    arrived = exchange(
        leaving.reshape(experts, picks_each, width), "ep", out_first
    ).reshape(count, width)

    packed = (model_width + model_width // 2, units)
    pack = pl.pallas_call(
        pack_kernel,
        out_shape=[bf16(packed)] * 2,
        in_specs=[HBM] * 3,
        out_specs=[HBM] * 2,
        scratch_shapes=[
            pltpu.VMEM((2, *packed), jnp.bfloat16),
            pltpu.SemaphoreType.DMA((2, 2 + model_width // units)),
            pltpu.SemaphoreType.DMA((2,)),
        ],
        compiler_params=room(6),
        cost_estimate=cost(10**8, 12 * model_width * units),
        name="pack",
    )
    packs = pack(in_hbm(gate), in_hbm(up), in_hbm(down))
    shared = [
        lax.ppermute(pack, ("ep", "tp"), neighbour_pairs(which, experts))
        for which, pack in enumerate(packs)
    ]

    place = pl.pallas_call(
        functools.partial(place_kernel, back_first),
        out_shape=bf16((3, tok_count, count)),
        in_specs=[HBM, VMEM],
        out_specs=VMEM,
        scratch_shapes=[pltpu.VMEM((picks_each, experts), jnp.int32), pltpu.SemaphoreType.DMA],
        compiler_params=room(4),
        cost_estimate=cost(10**8, 8 * tok_count * count),
        name="place",
    )
    places = place(by_pick, jnp.transpose(chosen_weight[0]))

    tiles = pl.pallas_call(
        spread_kernel,
        out_shape=bf16((tp_count, count // 2, width)),
        in_specs=[VMEM],
        out_specs=HBM,
        scratch_shapes=[pltpu.SemaphoreType.DMA((tp_count,))],
        compiler_params=room(2),
        cost_estimate=cost(10**8, tp_count * count * width),
        name="spread",
    )(arrived)
    tiles = exchange(tiles, "tp")
    partial = pl.pallas_call(
        ffn_kernel,
        out_shape=bf16((tp_count, count // 2, width)),
        in_specs=[ANY, VMEM, VMEM, HBM, HBM, HBM],
        out_specs=VMEM,
        scratch_shapes=[
            pltpu.VMEM((count // 2, model_width), jnp.bfloat16),
            pltpu.VMEM(packed, jnp.bfloat16),
            pltpu.VMEM(packed, jnp.bfloat16),
            pltpu.VMEM(down.shape, jnp.bfloat16),
            pltpu.SemaphoreType.DMA((tp_count,)),
            pltpu.SemaphoreType.DMA((3,)),
        ],
        cost_estimate=cost(6 * count * model_width * units, 12 * model_width * units),
        compiler_params=room(20),
        name="ffn",
    )(tiles, gate, up, in_hbm(down), *map(in_hbm, shared))
    partial = exchange(partial, "tp")
    expert_out = pl.pallas_call(
        functools.partial(sum_kernel, (back_first - out_first) * picks_each),
        out_shape=bf16((count, width)),
        in_specs=[VMEM],
        out_specs=VMEM,
        compiler_params=room(6),
        cost_estimate=cost(10**8, tp_count * count * width),
        name="add",
    )(partial)
    returned = exchange(
        expert_out.reshape(blocks, picks_each, width), "ep", back_first
    ).reshape(experts * picks_each, width)
    return pl.pallas_call(
        combine_kernel,
        out_shape=bf16((tok_count, width)),
        in_specs=[VMEM] * 2,
        out_specs=VMEM,
        compiler_params=room(4),
        cost_estimate=cost(6 * tok_count * count * width, 8 * tok_count * count),
        name="combine",
    )(places, returned)


def solution(mesh):
    return jax.shard_map(
        local,
        mesh=mesh,
        in_specs=(
            P("ep", None),
            P(),
            P("ep", None, None),
            P("ep", None, "tp"),
            P("ep", None, "tp"),
            P("ep", "tp", None),
        ),
        out_specs=P("ep", "tp"),
        check_vma=False,
    )
```
